32 devices in a mesh: fs: 8 (over z, x), tp: 4 (over y, core).
Axes of the slice: x: 2, y: 2, z: 4, core: 2. Of those that a mesh axis runs over, the one named last changes fastest.
Arguments:
- tokens: bfloat16 [1024, 2048], P('fs', 'tp'), may hold values from -6 to 6
- routes: int32 [1024, 2], P('fs'), may hold values from 0 to 3, all different within a row; in each aligned block of 128 rows (0 to 127, 128 to 255, ...) at most 96 rows name the same one
- route_weight: float32 [1024, 2], P('fs'), may hold values from 0.1 to 1
- norm_gain: float32 [2048], P('fs'), may hold values from 0.1 to 1.9
- expert_gate: float32 [4, 2048, 512], P(None, 'fs', 'tp'), may hold values from -0.125 to 0.125
- expert_up: float32 [4, 2048, 512], P(None, 'fs', 'tp'), may hold values from -0.125 to 0.125
- expert_down: float32 [4, 2048, 512], P(None, 'fs', 'tp'), may hold values from -0.25 to 0.25
- shared_gate: float32 [2048, 512], P('fs', 'tp'), may hold values from -0.125 to 0.125
- shared_up: float32 [2048, 512], P('fs', 'tp'), may hold values from -0.125 to 0.125
- shared_down: float32 [512, 2048], P('tp', 'fs'), may hold values from -0.25 to 0.25
Outputs:
- mixed: bfloat16 [1024, 2048], P('fs', 'tp')
- gate_sampler: bfloat16 [8, 2048, 256], P('fs', None, 'tp')
- up_sampler: bfloat16 [8, 2048, 256], P('fs', None, 'tp')
- down_sampler: bfloat16 [8, 2048, 256], P('fs', 'tp')
- shared_gate_out: bfloat16 [2048, 512], P(None, 'tp')
- shared_up_out: bfloat16 [2048, 512], P(None, 'tp')
- shared_down_out: bfloat16 [512, 2048], P('tp')
The draws below stay inside these ranges and needn't reach their ends.
Inputs may be any that keep to these rules, and one draw needn't show every extreme that they name: `routes`: each row names 2 different experts. In each aligned block of 128 rows no expert is named by more than 96 rows, a bound that some block reaches.
All inputs are finite; a program needn't handle non-finite values.
Results may differ from the reference program's by a relative error of at most 0.009.
Values may be sent and summed in bfloat16 or wider, within the bound.
A program may use at most 64 MiB of HBM per device.

```python
import math
import jax
import jax.numpy as jnp
import numpy as np
from jax import lax

D = 2048
FF = 512
TOP_K = 2
TOK_DEV = 128
EXPERTS = 4
UNITS = 64
SHARED_BLOCK = 128
CAP = 96
TOKENS = 1024
N_FS = 8
N_TP = 4


def steps_of(rng, shape, split, least, high):
    gain = 1.0
    for dim, blocks in split:
        heights = jax.random.uniform(jax.random.fold_in(jax.random.fold_in(rng, 6), dim), (blocks,), jnp.float32, least / len(split), high / len(split))
        gain = gain * jnp.repeat(jnp.exp(heights), shape[dim] // blocks).reshape((-1,) + (1,) * (len(shape) - 1 - dim))
    return gain


def routed_block(own_key, own, number, rows, number_of, top, most, slope):
    sequence = jax.random.permutation(own_key, number_of)
    heavy_load, ordinary = shares(number_of, rows * top, most, slope, True), shares(number_of, rows * top, most, slope, False)
    places = jnp.arange(number_of)

    def named(sizes, turn):
        used = int((sizes > 0).sum())
        fixed = max(1, used // 4)
        passed = fixed + (places - fixed + turn * (used - fixed)) % max(1, number_of - fixed)
        return jnp.zeros((number_of,), jnp.int32).at[sequence[jnp.where(places < fixed, places, passed)]].set(jnp.asarray(sizes, jnp.int32))

    sizes = jnp.where(number % 4 == 0, named(heavy_load, number // 4), named(ordinary, number - number // 4 - 1))
    mixed = jax.random.permutation(jax.random.fold_in(own, 3), number_of)
    giver, sink = mixed[0:number_of // 2 * 2:2], mixed[1:number_of // 2 * 2:2]
    margin = jnp.minimum(sizes[giver] - 1, most - sizes[sink]) // 2
    margin = jnp.where((giver == sequence[0]) | (sink == sequence[0]) | (sizes[sink] == 0), 0, jnp.maximum(margin, 0))
    passed = jax.random.randint(jax.random.fold_in(own, 4), (number_of // 2,), 0, 1 << 20) % (margin + 1)
    sizes = sizes.at[giver].add(-passed).at[sink].add(passed)
    items = jnp.searchsorted(jnp.cumsum(sizes), jnp.arange(rows * top), side="right").astype(jnp.int32)
    table = items.reshape(top, rows).T
    table = table[jax.random.permutation(jax.random.fold_in(own, 1), rows)]
    turn = jax.random.randint(jax.random.fold_in(own, 2), (rows, 1), 0, top)
    return jnp.take_along_axis(table, (jnp.arange(top)[None, :] + turn) % top, axis=1)


def shares(amount, total, limit, lean, full):
    portions = [(1 << 20) // math.isqrt(rank ** lean) + 1 for rank in range(1, amount + 1)]
    largest = limit if full else min(limit, max(-(-total // amount), total * portions[0] // sum(portions)))
    least = 1 if total - largest >= amount - 1 else 0
    given, rest = [largest] + [least] * (amount - 1), total - largest - least * (amount - 1)
    while rest > 0:
        movable = [i for i in range(1, amount) if given[i] < largest] or [i for i in range(1, amount) if given[i] < limit]
        mass, budget = sum([portions[i] for i in movable]), rest
        for i in movable:
            addition = min(limit - given[i], max(1, budget * portions[i] // mass), rest)
            given[i] = given[i] + addition
            rest = rest - addition
    return np.array(given)


def noise(stream_key, extent, width, bound, pieces=(), held_as=jnp.bfloat16):
    gain = steps_of(stream_key, extent, pieces, -0.22, 0.18) if pieces else 1.0
    values = jax.random.normal(stream_key, extent, jnp.float32) * width * gain
    return jnp.minimum(jnp.maximum(values, -bound), bound).astype(held_as)


def setup_inputs(seed: int = 0) -> dict:
    keys = jax.random.split(jax.random.key(seed), 11)
    tokens = noise(keys[0], (TOKENS, D), 1.0, 6.0, ((0, 8), (1, 4)))
    routes_keys = jax.random.split(jax.random.fold_in(keys[1], 1), TOKENS // TOK_DEV)
    routes_turns = jax.random.permutation(jax.random.fold_in(keys[1], 3), TOKENS // TOK_DEV)
    routes = jax.vmap(lambda own, number: routed_block(jax.random.fold_in(keys[1], 2), own, number, TOK_DEV, EXPERTS, TOP_K, CAP, 0))(routes_keys, routes_turns).reshape((TOKENS, TOP_K))
    route_weight = jnp.clip(0.1 + 0.9 * jax.random.uniform(keys[2], (TOKENS, TOP_K), jnp.float32) ** steps_of(keys[2], (TOKENS, TOP_K), ((0, 8),), -0.2, 0.2), 0.1, 1.0)
    norm_gain = jnp.clip(1.0 + 0.18 * jax.random.normal(keys[3], (D,), jnp.float32), 0.1, 1.9)
    expert_gate = noise(keys[4], (EXPERTS, D, FF), D ** -0.5, 0.125, ((1, 8), (2, 4)), jnp.float32)
    expert_up = noise(keys[5], (EXPERTS, D, FF), D ** -0.5, 0.125, ((1, 8), (2, 4)), jnp.float32)
    expert_down = noise(keys[6], (EXPERTS, D, FF), FF ** -0.5, 0.25, ((1, 8), (2, 4)), jnp.float32)
    shared_gate = noise(keys[7], (D, FF), D ** -0.5, 0.125, ((0, 8), (1, 4)), jnp.float32)
    shared_up = noise(keys[8], (D, FF), D ** -0.5, 0.125, ((0, 8), (1, 4)), jnp.float32)
    shared_down = noise(keys[9], (FF, D), FF ** -0.5, 0.25, ((0, 4), (1, 8)), jnp.float32)
    return {"tokens": tokens, "routes": routes, "route_weight": route_weight, "norm_gain": norm_gain, "expert_gate": expert_gate, "expert_up": expert_up, "expert_down": expert_down, "shared_gate": shared_gate, "shared_up": shared_up, "shared_down": shared_down}


EPS = 1e-06

def slot_places(routes):
    blocks = routes.reshape(N_FS, TOK_DEV * TOP_K)
    onehot = (blocks[:, :, None] == jnp.arange(EXPERTS, dtype=jnp.int32)[None, None, :]).astype(jnp.int32)
    earlier = jnp.cumsum(onehot, axis=1) - onehot
    position = lax.optimization_barrier(jnp.sum(earlier * onehot, axis=2))
    return (blocks * CAP + position).astype(jnp.int32)

def to_sampler(folded):
    return folded.reshape(EXPERTS, D, N_TP, 2, UNITS).transpose(0, 3, 1, 2, 4).reshape(2 * EXPERTS, D, N_TP * UNITS)

def reference(tokens, routes, route_weight, norm_gain, expert_gate, expert_up, expert_down, shared_gate, shared_up, shared_down):
    gate_folded = (expert_gate * norm_gain[None, :, None]).astype(jnp.bfloat16)
    up_folded = (expert_up * norm_gain[None, :, None]).astype(jnp.bfloat16)
    down_round = expert_down.astype(jnp.bfloat16)
    gate_sampler = to_sampler(gate_folded)
    up_sampler = to_sampler(up_folded)
    down_sampler = to_sampler(down_round)
    shared_gate_out = (shared_gate * norm_gain[:, None]).astype(jnp.bfloat16)
    shared_up_out = (shared_up * norm_gain[:, None]).astype(jnp.bfloat16)
    shared_down_out = shared_down.astype(jnp.bfloat16)
    tokens_wide = tokens.astype(jnp.float32)
    normed = (tokens_wide * lax.rsqrt(lax.optimization_barrier(jnp.mean(tokens_wide * tokens_wide, axis=1, keepdims=True)) + EPS)).astype(jnp.bfloat16)
    shared_act = jnp.dot(normed, shared_gate_out, preferred_element_type=jnp.float32)
    shared_lin = jnp.dot(normed, shared_up_out, preferred_element_type=jnp.float32)
    shared_hidden = (jax.nn.silu(shared_act) * shared_lin).astype(jnp.bfloat16)
    shared_sum = jnp.zeros((TOKENS, D), jnp.float32)
    for tp_part in range(N_TP):
        lower = tp_part * SHARED_BLOCK
        product = jnp.dot(shared_hidden[:, lower:lower + SHARED_BLOCK], shared_down_out[lower:lower + SHARED_BLOCK], preferred_element_type=jnp.float32)
        shared_sum = shared_sum + lax.optimization_barrier(product.astype(jnp.bfloat16)).astype(jnp.float32)
    places = slot_places(routes)
    block_ids = jnp.arange(N_FS, dtype=jnp.int32)[:, None]
    token_ids = (block_ids * TOK_DEV + jnp.arange(TOK_DEV * TOP_K, dtype=jnp.int32)[None, :] // TOP_K).astype(jnp.int32)
    slot_table = jnp.full((N_FS, EXPERTS * CAP), TOKENS, jnp.int32).at[block_ids, places].set(token_ids)
    slot_weight = jnp.zeros((N_FS, EXPERTS * CAP), jnp.float32).at[block_ids, places].set(route_weight.reshape(N_FS, TOK_DEV * TOP_K))
    slot_table = slot_table.reshape(N_FS, EXPERTS, CAP).transpose(1, 0, 2).reshape(EXPERTS, N_FS * CAP)
    slot_weight = slot_weight.reshape(N_FS, EXPERTS, CAP).transpose(1, 0, 2).reshape(EXPERTS, N_FS * CAP)
    padded = jnp.concatenate([normed, jnp.zeros((1, D), jnp.bfloat16)], axis=0)

    def expert_step(totals, inputs):
        row_ids, weights, gate_rows, up_rows, down_rows = inputs
        picked = padded[row_ids]
        gate_act = jnp.dot(picked, gate_rows, preferred_element_type=jnp.float32)
        up_act = jnp.dot(picked, up_rows, preferred_element_type=jnp.float32)
        hidden = (jax.nn.silu(gate_act) * up_act).astype(jnp.bfloat16).reshape(N_FS * CAP, N_TP, 2, UNITS)
        down_parts = down_rows.reshape(D, N_TP, 2, UNITS)
        combined = jnp.zeros((N_FS * CAP, D), jnp.float32)
        for half_index in range(2):
            down_half = down_parts[:, :, half_index, :].reshape(D, N_TP * UNITS)
            product = jnp.dot(hidden[:, :, half_index, :].reshape(N_FS * CAP, N_TP * UNITS), down_half.T, preferred_element_type=jnp.float32)
            combined = combined + lax.optimization_barrier(product.astype(jnp.bfloat16)).astype(jnp.float32)
        return (totals.at[row_ids].add(combined * weights[:, None]), None)
    routed_total, _ = lax.scan(expert_step, jnp.zeros((TOKENS + 1, D), jnp.float32), (slot_table, slot_weight, gate_folded, up_folded, down_round))
    mixed = (shared_sum + routed_total[:TOKENS]).astype(jnp.bfloat16)
    return (mixed, gate_sampler, up_sampler, down_sampler, shared_gate_out, shared_up_out, shared_down_out)
```

```python
import functools

import jax
import jax.numpy as jnp
from jax import lax
from jax.experimental import pallas as pl
from jax.experimental.pallas import tpu as pltpu
from jax.sharding import PartitionSpec as P

EPS = 1e-06
BF = jnp.bfloat16
F32 = jnp.float32


def loop(low, high, body):
    def step(i, carry):
        body(i)
        return carry

    lax.fori_loop(low, high, step, 0)


def dot(a, b):
    return jnp.dot(a, b, preferred_element_type=F32)


def dot_nt(a, b):
    return lax.dot_general(a, b, (((1,), (1,)), ((), ())), preferred_element_type=F32)


def left_halves(a, b, half):
    lane = lax.broadcasted_iota(jnp.int32, a.shape, 1)
    return jnp.where(lane < half, a, pltpu.roll(b, half, 1))


def right_halves(a, b, half):
    lane = lax.broadcasted_iota(jnp.int32, a.shape, 1)
    return jnp.where(lane < half, pltpu.roll(a, half, 1), b)


def silu(v):
    return v / (1.0 + jnp.exp(-v))


def kernel(
    F,
    T,
    slots,
    tok,
    routes,
    weight,
    gain,
    eg,
    eu,
    ed,
    sg,
    su,
    sd,
    mixed,
    gu_out,
    dn_out,
    sg_out,
    su_out,
    sd_out,
    tk,
    nm,
    gu_send,
    gu,
    dn_send,
    dn,
    sh,
    disp,
    port,
    hid,
    ret_send,
    ret,
    part,
    shr,
    s_tok,
    r_tok,
    s_gu,
    r_gu,
    s_dn,
    r_dn,
    s_sha,
    s_shb,
    r_sh,
    s_da,
    s_db,
    s_out,
    s_in,
    r_port,
    s_hid,
    r_hid,
    s_ret,
    r_ret,
    s_shr,
    r_shr,
):
    G = F // 2
    K = F // T
    E = eg.shape[0]
    R, C = eg.shape[1], eg.shape[2]
    half = C // 2
    tok_count = tok.shape[0]
    quarter = tok.shape[1]
    width = quarter * T
    f = lax.axis_index("fs")
    t = lax.axis_index("tp")
    g, p = f // 2, f % 2
    pair = g * 2 + (1 - p)
    t_pair = (t // 2) * 2 + (1 - t % 2)

    def remote(src, dst, send, recv, fs, tp):
        return pltpu.make_async_remote_copy(
            src_ref=src,
            dst_ref=dst,
            send_sem=send,
            recv_sem=recv,
            device_id={"fs": fs, "tp": tp},
            device_id_type=pl.DeviceIdType.MESH,
        )

    def arrived(dst, send, recv):
        remote(dst, dst, send, recv, pair, t).wait_recv()

    def sent(src, send, recv):
        remote(src, src, send, recv, pair, t).wait_send()

    def send_tok(d):
        remote(tok, tk.at[t], s_tok.at[d], r_tok.at[t], f, (t + d) % T).start()

    loop(1, T, send_tok)
    tk[t] = tok[...]

    gains = gain[...]

    def fold(e):
        gate, up = eg[e] * gains, eu[e] * gains
        gu_send[2 * e] = left_halves(gate, up, half).astype(BF)
        gu_send[2 * e + 1] = right_halves(gate, up, half).astype(BF)

    loop(0, E, fold)
    gu[f] = gu_send[f]

    def send_gu(d):
        j = (f + d) % F
        remote(gu_send.at[j], gu.at[f], s_gu.at[d], r_gu.at[f], j, t).start()

    loop(1, F, send_gu)

    def fold_down(e):
        top, low = ed[e, : R // 2], ed[e, R // 2 :]
        dn_send[2 * e] = left_halves(top, low, half).astype(BF)
        dn_send[2 * e + 1] = right_halves(top, low, half).astype(BF)

    loop(0, E, fold_down)
    sh[f, 0] = (sg[...] * gains).astype(BF)
    sh[f, 1] = (su[...] * gains).astype(BF)
    sh[f, 2] = sd[...].T.astype(BF)

    experts = lax.broadcasted_iota(jnp.int32, (tok_count, E), 1)
    first, second = routes[:, 0:1], routes[:, 1:2]
    named = ((experts == first) | (experts == second)).astype(F32)
    rows = lax.broadcasted_iota(jnp.int32, (tok_count, tok_count), 0)
    cols = lax.broadcasted_iota(jnp.int32, (tok_count, tok_count), 1)
    before = (cols < rows).astype(F32).astype(BF)
    place = dot(before, named.astype(BF))
    slot_ids = lax.broadcasted_iota(jnp.int32, (tok_count, E * slots), 1)

    def pick_of(chosen):
        spot = jnp.sum(jnp.where(experts == chosen, place, 0.0), axis=1, keepdims=True)
        return slot_ids == chosen * slots + spot.astype(jnp.int32)

    pick0, pick1 = pick_of(first), pick_of(second)
    both = jnp.where(pick0 | pick1, 1.0, 0.0).astype(BF)

    def wait_tok(d):
        src = (t + d) % T
        arrived(tk.at[src], s_tok.at[d], r_tok.at[src])

    loop(1, T, wait_tok)
    squares = jnp.zeros((tok_count, 1), F32)
    for q in range(T):
        x = tk[q].astype(F32)
        squares = squares + jnp.sum(x * x, axis=1, keepdims=True)
    scale = lax.rsqrt(squares / width + EPS)
    for q in range(T):
        nm[q] = (tk[q].astype(F32) * scale).astype(BF)

    packed = lax.dot_general(
        both, nm[t], (((0,), (0,)), ((), ())), preferred_element_type=F32
    ).astype(BF)
    disp[...] = packed.reshape(E, slots, quarter)
    port[t, f] = disp[g]

    def send_disp(d):
        e = (g + d) % G
        remote(
            disp.at[e], port.at[t, f], s_da.at[d], r_port.at[t, f], 2 * e + p, t
        ).start()

    loop(1, G, send_disp)

    def send_shared(d):
        remote(
            sh.at[f], sh.at[f], s_sha.at[d], r_sh.at[f], ((g + d) % G) * 2 + p, t
        ).start()

    def pass_block(block):
        for d in range(1, T // 2):
            remote(
                port.at[t, block],
                port.at[t, block],
                s_out.at[d, block],
                r_port.at[t, block],
                f,
                (t + 2 * d) % T,
            ).start()
        remote(
            port.at[t, block],
            port.at[t, block],
            s_in.at[0, block],
            r_port.at[t, block],
            f,
            t_pair,
        ).start()

    def direct_block(d):
        block = ((g + d) % G) * 2 + p

        @pl.when(d > 0)
        def _():
            arrived(port.at[t, block], s_da.at[d], r_port.at[t, block])

        remote(
            port.at[t, block],
            port.at[t, block],
            s_db.at[d],
            r_port.at[t, block],
            pair,
            t,
        ).start()
        pass_block(block)

    def pair_block(d):
        block = ((g + d) % G) * 2 + 1 - p
        arrived(port.at[t, block], s_db.at[d], r_port.at[t, block])
        pass_block(block)

    def inner_block(d):
        for o in range(1, T // 2):
            src = (t + 2 * o) % T
            for q in (p, 1 - p):
                block = ((g + d) % G) * 2 + q
                arrived(port.at[src, block], s_out.at[o, block], r_port.at[src, block])
                remote(
                    port.at[src, block],
                    port.at[src, block],
                    s_in.at[o, block],
                    r_port.at[src, block],
                    f,
                    t_pair,
                ).start()

    def down_copy(d):
        j = (f + d) % F
        return remote(
            dn_send.at[j], dn.at[f % K, t], s_dn.at[d], r_dn.at[f % K, t], j, f // K
        )

    mine = f // K == t

    @pl.when(mine)
    def _():
        dn[f % K, t] = dn_send[f]

    def send_down(d):
        @pl.when(jnp.logical_not((d == 0) & mine))
        def _():
            down_copy(d).start()

    loop(0, F, send_down)
    loop(1, G, send_shared)
    remote(sh.at[f], sh.at[f], s_shb.at[0], r_sh.at[f], pair, t).start()
    loop(0, G, direct_block)
    loop(0, G, pair_block)

    def pass_shared(d):
        block = ((g + d) % G) * 2 + p
        arrived(sh.at[block], s_sha.at[d], r_sh.at[block])
        remote(sh.at[block], sh.at[block], s_shb.at[d], r_sh.at[block], pair, t).start()

    loop(1, G, pass_shared)
    loop(0, G, inner_block)

    def wait_shared(d):
        block = ((g + d) % G) * 2 + 1 - p
        arrived(sh.at[block], s_shb.at[d], r_sh.at[block])

    loop(0, G, wait_shared)

    gate_sh = sh[:, 0].reshape(F * R, C)
    up_sh = sh[:, 1].reshape(F * R, C)
    down_sh = sh[:, 2].reshape(F * R, C)
    sg_out[...] = gate_sh
    su_out[...] = up_sh
    sd_out[...] = down_sh.astype(F32).T.astype(BF)
    act = jnp.zeros((tok_count, C), F32)
    lin = jnp.zeros((tok_count, C), F32)
    for q in range(T):
        act = act + dot(nm[q], gate_sh[q * quarter : (q + 1) * quarter])
        lin = lin + dot(nm[q], up_sh[q * quarter : (q + 1) * quarter])
    hidden_sh = (silu(act) * lin).astype(BF)
    for q in range(T):
        part[q] = dot_nt(hidden_sh, down_sh[q * quarter : (q + 1) * quarter]).astype(BF)
    shr[t] = part[t]

    def send_part(d):
        q = (t + d) % T
        remote(part.at[q], shr.at[t], s_shr.at[d], r_shr.at[t], f, q).start()

    loop(1, T, send_part)

    def wait_gu(d):
        src = (f + d) % F
        arrived(gu.at[src], s_gu.at[d], r_gu.at[src])

    loop(1, F, wait_gu)
    gu_out[...] = gu[...].reshape(F * R, C)

    def hidden_of(block):
        total = jnp.zeros((slots, C), F32)
        for q in range(T):
            total = total + dot(port[q, block], gu_out[q * quarter : (q + 1) * quarter, :])
        return silu(total) * pltpu.roll(total, half, 1)

    def wait_inner(block):
        for o in range(T // 2):
            src = (t_pair + 2 * o) % T
            arrived(port.at[src, block], s_in.at[o, block], r_port.at[src, block])

    def expert_hidden(d):
        group = (g + d) % G
        wait_inner(2 * group)
        wait_inner(2 * group + 1)
        hid[t, group] = left_halves(
            hidden_of(2 * group), hidden_of(2 * group + 1), half
        ).astype(BF)
        for o in range(1, T):
            remote(
                hid.at[t, group],
                hid.at[t, group],
                s_hid.at[o, group],
                r_hid.at[t, group],
                f,
                (t + o) % T,
            ).start()

    loop(0, G, expert_hidden)

    def wait_down(k):
        for q in range(T):

            @pl.when(jnp.logical_not((t * K + k == f) & (t == q)))
            def _():
                arrived(dn.at[k, q], s_dn.at[0], r_dn.at[k, q])

    loop(0, K, wait_down)

    def place_down(k):
        for q in range(0, T, 2):
            a, b = dn[k, q].astype(F32), dn[k, q + 1].astype(F32)
            block = jnp.concatenate([left_halves(a, b, half), right_halves(a, b, half)], axis=0)
            dn_out[pl.ds(pl.multiple_of(k * R, R), R), q * half : (q + 2) * half] = block.astype(BF)

    loop(0, K, place_down)

    def ret_copy(d, q):
        block = ((g + d) % G) * 2 + q
        return block, remote(
            ret_send.at[block], ret.at[p, g], s_ret.at[block], r_ret.at[p, g], block, t
        )

    def expert_out(d):
        group = (g + d) % G
        for o in range(1, T):
            src = (t + o) % T
            arrived(hid.at[src, group], s_hid.at[o, group], r_hid.at[src, group])
        out_a = jnp.zeros((slots, quarter), F32)
        out_b = jnp.zeros((slots, quarter), F32)
        for q in range(0, T, 2):
            a, b = hid[q, group].astype(F32), hid[q + 1, group].astype(F32)
            down = dn_out[:, q * half : (q + 2) * half]
            out_a = out_a + dot_nt(left_halves(a, b, half).astype(BF), down)
            out_b = out_b + dot_nt(right_halves(a, b, half).astype(BF), down)
        ret_send[2 * group] = out_a.astype(BF)
        ret_send[2 * group + 1] = out_b.astype(BF)
        for q in range(2):
            block, copy = ret_copy(d, q)

            @pl.when(block != f)
            def _():
                copy.start()

    loop(0, G, expert_out)
    ret[p, g] = ret_send[f]

    def wait_part(d):
        src = (t + d) % T
        arrived(shr.at[src], s_shr.at[d], r_shr.at[src])

    loop(1, T, wait_part)
    total = shr[0].astype(F32)
    for q in range(1, T):
        total = total + shr[q].astype(F32)

    def wait_ret(d):
        src = (f + d) % F
        arrived(ret.at[src % 2, src // 2], s_ret.at[src], r_ret.at[src % 2, src // 2])

    loop(1, F, wait_ret)
    for k, pick in enumerate((pick0, pick1)):
        chosen = jnp.where(pick, 1.0, 0.0).astype(BF)
        halves = dot(chosen, ret[0].reshape(E * slots, quarter)) + dot(
            chosen, ret[1].reshape(E * slots, quarter)
        )
        total = total + weight[:, k : k + 1] * halves
    mixed[...] = total.astype(BF)

    def done_tp(d):
        sent(tok, s_tok.at[d], r_tok.at[0])
        sent(part.at[0], s_shr.at[d], r_shr.at[0])

        def inner(group):
            sent(hid.at[t, group], s_hid.at[d, group], r_hid.at[0, 0])

        loop(0, G, inner)

    loop(1, T, done_tp)

    def done_fs(d):
        sent(gu_send.at[0], s_gu.at[d], r_gu.at[0])
        sent(ret_send.at[0], s_ret.at[(f + d) % F], r_ret.at[0, 0])

    loop(1, F, done_fs)

    def done_down(d):
        @pl.when(jnp.logical_not((d == 0) & mine))
        def _():
            sent(dn_send.at[0], s_dn.at[d], r_dn.at[0, 0])

    loop(0, F, done_down)

    def done_groups(d):
        sent(sh.at[f], s_shb.at[d], r_sh.at[0])
        sent(disp.at[0], s_db.at[d], r_port.at[0, 0])

        @pl.when(d > 0)
        def _():
            sent(sh.at[f], s_sha.at[d], r_sh.at[0])
            sent(disp.at[0], s_da.at[d], r_port.at[0, 0])

    loop(0, G, done_groups)

    def done_blocks(block):
        for o in range(T // 2):
            sent(disp.at[0], s_in.at[o, block], r_port.at[0, 0])
            if o > 0:
                sent(disp.at[0], s_out.at[o, block], r_port.at[0, 0])

    loop(0, F, done_blocks)


def on_device(
    tokens,
    routes,
    route_weight,
    norm_gain,
    expert_gate,
    expert_up,
    expert_down,
    shared_gate,
    shared_up,
    shared_down,
):
    F = lax.axis_size("fs")
    T = lax.axis_size("tp")
    E, R, C = expert_gate.shape
    tok_count, quarter = tokens.shape
    pick_count = routes.shape[1]
    capacity = 2 * ((3 * tok_count * pick_count + 4 * E - 1) // (4 * E))
    slots = (capacity + 15) // 16 * 16
    G, K = F // 2, F // T
    vmem = pl.BlockSpec(memory_space=pltpu.VMEM)
    dma = pltpu.SemaphoreType.DMA
    shapes = [
        (tok_count, quarter),
        (F * R, C),
        (K * R, T * C // 2),
        (F * R, C),
        (F * R, C),
        (C, F * R),
    ]
    scratch = [
        (T, tok_count, quarter),
        (T, tok_count, quarter),
        (F, R, C),
        (F, R, C),
        (F, R // 2, C),
        (K, T, R // 2, C),
        (F, 3, R, C),
        (E, slots, quarter),
        (T, F, slots, quarter),
        (T, G, slots, C),
        (F, slots, quarter),
        (2, E, slots, quarter),
        (T, tok_count, quarter),
        (T, tok_count, quarter),
    ]
    sems = [
        (T,), (T,), (F,), (F,), (F,), (K, T), (G,), (G,), (F,), (G,), (G,),
        (T // 2, F), (T // 2, F), (T, F), (T, G), (T, G), (F,), (2, E), (T,), (T,),
    ]
    mixed, gu, down, sg, su, sd = pl.pallas_call(
        functools.partial(kernel, F, T, slots),
        out_shape=[jax.ShapeDtypeStruct(s, BF) for s in shapes],
        in_specs=[vmem] * 10,
        out_specs=[vmem] * 6,
        scratch_shapes=[pltpu.VMEM(s, BF) for s in scratch] + [dma(s) for s in sems],
        compiler_params=pltpu.CompilerParams(
            has_side_effects=True, vmem_limit_bytes=60 * 1024 * 1024
        ),
    )(
        tokens,
        routes,
        route_weight,
        norm_gain[:, None],
        expert_gate,
        expert_up,
        expert_down,
        shared_gate,
        shared_up,
        shared_down,
    )
    return (mixed, gu[None, :, : C // 2], gu[None, :, C // 2 :], down[None], sg, su, sd)


def solution(mesh):
    in_specs = (
        P("fs", "tp"),
        P("fs", None),
        P("fs", None),
        P("fs"),
        P(None, "fs", "tp"),
        P(None, "fs", "tp"),
        P(None, "fs", "tp"),
        P("fs", "tp"),
        P("fs", "tp"),
        P("tp", "fs"),
    )
    out_specs = (
        P("fs", "tp"),
        P("fs", None, "tp"),
        P("fs", None, "tp"),
        P("fs", "tp", None),
        P(None, "tp"),
        P(None, "tp"),
        P("tp", None),
    )
    return jax.shard_map(
        on_device, mesh=mesh, in_specs=in_specs, out_specs=out_specs, check_vma=False
    )
```

```python
import functools

import jax
import jax.numpy as jnp
from jax import lax
from jax.experimental import pallas as pl
from jax.experimental.pallas import tpu as pltpu
from jax.sharding import PartitionSpec as P

EPS = 1e-06
BF = jnp.bfloat16
F32 = jnp.float32


def loop(low, high, body):
    def step(i, carry):
        body(i)
        return carry

    lax.fori_loop(low, high, step, 0)


def dot(a, b):
    return jnp.dot(a, b, preferred_element_type=F32)


def dot_nt(a, b):
    return lax.dot_general(a, b, (((1,), (1,)), ((), ())), preferred_element_type=F32)


def left_halves(a, b, half):
    lane = lax.broadcasted_iota(jnp.int32, a.shape, 1)
    return jnp.where(lane < half, a, pltpu.roll(b, half, 1))


def right_halves(a, b, half):
    lane = lax.broadcasted_iota(jnp.int32, a.shape, 1)
    return jnp.where(lane < half, pltpu.roll(a, half, 1), b)


def silu(v):
    return v / (1.0 + jnp.exp(-v))


def kernel(
    F,
    T,
    slots,
    tok,
    routes,
    weight,
    gain,
    eg,
    eu,
    ed,
    sg,
    su,
    sd,
    mixed,
    gate_out,
    up_out,
    dn_out,
    sg_out,
    su_out,
    sd_out,
    tk,
    nm,
    gu_send,
    gu,
    dn_send,
    dn,
    sh,
    disp,
    port,
    hid,
    away,
    keep,
    near,
    ret_send,
    ret,
    part,
    shr,
    s_tok,
    r_tok,
    s_gu,
    r_gu,
    s_dn,
    r_dn,
    s_left,
    s_right,
    s_shb,
    r_sh,
    s_da,
    s_db,
    s_out,
    s_in,
    r_port,
    s_hid,
    r_hid,
    s_near,
    r_near,
    s_ret,
    r_ret,
    s_shr,
    r_shr,
):
    G = F // 2
    K = F // T
    E = eg.shape[0]
    R, C = eg.shape[1], eg.shape[2]
    half = C // 2
    tok_count = tok.shape[0]
    quarter = tok.shape[1]
    width = quarter * T
    f = lax.axis_index("fs")
    t = lax.axis_index("tp")
    g, p = f // 2, f % 2
    pair = g * 2 + (1 - p)
    t_pair = (t // 2) * 2 + (1 - t % 2)

    def remote(src, dst, send, recv, fs, tp):
        return pltpu.make_async_remote_copy(
            src_ref=src,
            dst_ref=dst,
            send_sem=send,
            recv_sem=recv,
            device_id={"fs": fs, "tp": tp},
            device_id_type=pl.DeviceIdType.MESH,
        )

    def arrived(dst, send, recv):
        remote(dst, dst, send, recv, pair, t).wait_recv()

    def sent(src, send, recv):
        remote(src, src, send, recv, pair, t).wait_send()

    def send_tok(d):
        remote(tok, tk.at[t], s_tok.at[d], r_tok.at[t], f, (t + d) % T).start()

    loop(1, T, send_tok)
    tk[t] = tok[...]

    gains = jnp.broadcast_to(gain[...], (8, R)).T[:, 0:1]

    def fold(e):
        gate, up = eg[e] * gains, eu[e] * gains
        gu_send[2 * e] = left_halves(gate, up, half).astype(BF)
        gu_send[2 * e + 1] = right_halves(gate, up, half).astype(BF)

    loop(0, E, fold)
    gu[f] = gu_send[f]

    def send_gu(d):
        j = (f + d) % F
        remote(gu_send.at[j], gu.at[f], s_gu.at[d], r_gu.at[f], j, t).start()

    loop(1, F, send_gu)

    def fold_down(e):
        top, low = ed[e, : R // 2], ed[e, R // 2 :]
        dn_send[2 * e] = left_halves(top, low, half).astype(BF)
        dn_send[2 * e + 1] = right_halves(top, low, half).astype(BF)

    loop(0, E, fold_down)
    sh[f, 0] = (sg[...] * gains).astype(BF)
    sh[f, 1] = (su[...] * gains).astype(BF)
    sh[f, 2] = sd[...].T.astype(BF)

    experts = lax.broadcasted_iota(jnp.int32, (tok_count, E), 1)
    line = lax.broadcasted_iota(jnp.int32, (8, tok_count), 0)
    named_by = routes[...].astype(F32)
    turned = jnp.where(line == 0, named_by[0:1], named_by[1:2])
    turned = jnp.where(line == 2, weight[0:1, :], turned)
    turned = jnp.where(line == 3, weight[1:2, :], turned).T
    first, second = turned[:, 0:1].astype(jnp.int32), turned[:, 1:2].astype(jnp.int32)
    named = ((experts == first) | (experts == second)).astype(F32)
    rows = lax.broadcasted_iota(jnp.int32, (tok_count, tok_count), 0)
    cols = lax.broadcasted_iota(jnp.int32, (tok_count, tok_count), 1)
    before = (cols < rows).astype(F32).astype(BF)
    place = dot(before, named.astype(BF))
    slot_ids = lax.broadcasted_iota(jnp.int32, (tok_count, E * slots), 1)

    def pick_of(chosen):
        spot = jnp.sum(jnp.where(experts == chosen, place, 0.0), axis=1, keepdims=True)
        return slot_ids == chosen * slots + spot.astype(jnp.int32)

    pick0, pick1 = pick_of(first), pick_of(second)
    both = jnp.where(pick0 | pick1, 1.0, 0.0).astype(BF)

    def wait_tok(d):
        src = (t + d) % T
        arrived(tk.at[src], s_tok.at[d], r_tok.at[src])

    loop(1, T, wait_tok)
    squares = jnp.zeros((tok_count, 1), F32)
    for q in range(T):
        x = tk[q].astype(F32)
        squares = squares + jnp.sum(x * x, axis=1, keepdims=True)
    scale = lax.rsqrt(squares / width + EPS)
    for q in range(T):
        nm[q] = (tk[q].astype(F32) * scale).astype(BF)

    packed = lax.dot_general(
        both, nm[t], (((0,), (0,)), ((), ())), preferred_element_type=F32
    ).astype(BF)
    disp[...] = packed.reshape(E, slots, quarter)
    port[t, f] = disp[g]

    def send_disp(d):
        e = (g + d) % G
        remote(
            disp.at[e], port.at[t, f], s_da.at[d], r_port.at[t, f], 2 * e + p, t
        ).start()

    loop(1, G, send_disp)

    def shared_copy(block, sems, to):
        return remote(sh.at[block], sh.at[block], sems, r_sh.at[block], to, t)

    def share_left(block):
        @pl.when(g > 0)
        def _():
            shared_copy(block, s_left.at[block // 2], f - 2).start()

    def share_right(block):
        @pl.when(g < G - 1)
        def _():
            shared_copy(block, s_right.at[block // 2], f + 2).start()

    def share_pair(block):
        shared_copy(block, s_shb.at[block // 2], pair).start()

    def relay(k):
        @pl.when(g - k >= 0)
        def _():
            block = f - 2 * k
            arrived(sh.at[block], s_right.at[0], r_sh.at[block])
            share_right(block)
            share_pair(block)

        @pl.when(g + k < G)
        def _():
            block = f + 2 * k
            arrived(sh.at[block], s_left.at[0], r_sh.at[block])
            share_left(block)
            share_pair(block)

    def pass_block(block):
        for d in range(1, T // 2):
            remote(
                port.at[t, block],
                port.at[t, block],
                s_out.at[d, block],
                r_port.at[t, block],
                f,
                (t + 2 * d) % T,
            ).start()
        remote(
            port.at[t, block],
            port.at[t, block],
            s_in.at[0, block],
            r_port.at[t, block],
            f,
            t_pair,
        ).start()

    def direct_block(d):
        block = ((g + d) % G) * 2 + p

        @pl.when(d > 0)
        def _():
            arrived(port.at[t, block], s_da.at[d], r_port.at[t, block])

        remote(
            port.at[t, block],
            port.at[t, block],
            s_db.at[d],
            r_port.at[t, block],
            pair,
            t,
        ).start()
        pass_block(block)

    def pair_block(d):
        block = ((g + d) % G) * 2 + 1 - p
        arrived(port.at[t, block], s_db.at[d], r_port.at[t, block])
        pass_block(block)

    def inner_block(d):
        for o in range(1, T // 2):
            src = (t + 2 * o) % T
            for q in (p, 1 - p):
                block = ((g + d) % G) * 2 + q
                arrived(port.at[src, block], s_out.at[o, block], r_port.at[src, block])
                remote(
                    port.at[src, block],
                    port.at[src, block],
                    s_in.at[o, block],
                    r_port.at[src, block],
                    f,
                    t_pair,
                ).start()

    def down_copy(d):
        j = (f + d) % F
        return remote(
            dn_send.at[j], dn.at[f % K, t], s_dn.at[d], r_dn.at[f % K, t], j, f // K
        )

    mine = f // K == t

    @pl.when(mine)
    def _():
        dn[f % K, t] = dn_send[f]

    def send_down(d):
        @pl.when(jnp.logical_not((d == 0) & mine))
        def _():
            down_copy(d).start()

    share_left(f)
    share_right(f)
    loop(0, F, send_down)
    loop(0, G, direct_block)
    loop(0, G, pair_block)
    share_pair(f)
    relay(1)
    loop(0, G, inner_block)
    def wait_gu(d):
        src = (f + d) % F
        arrived(gu.at[src], s_gu.at[d], r_gu.at[src])

    loop(1, F, wait_gu)

    def rows_of(q):
        return gu[q * K : (q + 1) * K].reshape(quarter, C)

    def hidden_of(block):
        total = jnp.zeros((slots, C), F32)
        for q in range(T):
            total = total + dot(port[q, block], rows_of(q))
        return silu(total) * pltpu.roll(total, half, 1)

    def wait_inner(block):
        for o in range(T // 2):
            src = (t_pair + 2 * o) % T
            arrived(port.at[src, block], s_in.at[o, block], r_port.at[src, block])

    def expert_hidden(d):
        group = (g + d) % G
        wait_inner(2 * group)
        wait_inner(2 * group + 1)
        hid[t, group] = left_halves(
            hidden_of(2 * group), hidden_of(2 * group + 1), half
        ).astype(BF)
        for o in range(1, T):
            remote(
                hid.at[t, group],
                hid.at[t, group],
                s_hid.at[o, group],
                r_hid.at[t, group],
                f,
                (t + o) % T,
            ).start()

    loop(0, G, expert_hidden)

    def wait_shared(d):
        block = ((g + d) % G) * 2 + 1 - p
        arrived(sh.at[block], s_shb.at[d], r_sh.at[block])

    loop(2, G, relay)
    loop(0, G, wait_shared)

    gate_sh = sh[:, 0].reshape(F * R, C)
    up_sh = sh[:, 1].reshape(F * R, C)
    down_sh = sh[:, 2].reshape(F * R, C)
    act = jnp.zeros((tok_count, C), F32)
    lin = jnp.zeros((tok_count, C), F32)
    for q in range(T):
        act = act + dot(nm[q], gate_sh[q * quarter : (q + 1) * quarter])
        lin = lin + dot(nm[q], up_sh[q * quarter : (q + 1) * quarter])
    hidden_sh = (silu(act) * lin).astype(BF)
    for q in range(T):
        part[q] = dot_nt(hidden_sh, down_sh[q * quarter : (q + 1) * quarter]).astype(BF)
    shr[t] = part[t]

    def send_part(d):
        q = (t + d) % T
        remote(part.at[q], shr.at[t], s_shr.at[d], r_shr.at[t], f, q).start()

    loop(1, T, send_part)

    def wait_down(k):
        for q in range(T):

            @pl.when(jnp.logical_not((t * K + k == f) & (t == q)))
            def _():
                arrived(dn.at[k, q], s_dn.at[0], r_dn.at[k, q])

    loop(0, K, wait_down)

    def place_down(k):
        for q in range(0, T, 2):
            a, b = dn[k, q].astype(F32), dn[k, q + 1].astype(F32)
            block = jnp.concatenate([left_halves(a, b, half), right_halves(a, b, half)], axis=0)
            dn_out[pl.ds(pl.multiple_of(k * R, R), R), q * half : (q + 2) * half] = block.astype(BF)

    loop(0, K, place_down)

    def near_copy(group):
        return remote(
            away.at[group], near.at[group], s_near.at[group], r_near.at[group], pair, t
        )

    def expert_out(d):
        group = (g + d) % G
        for o in range(1, T):
            src = (t + o) % T
            arrived(hid.at[src, group], s_hid.at[o, group], r_hid.at[src, group])
        out_a = jnp.zeros((slots, quarter), F32)
        out_b = jnp.zeros((slots, quarter), F32)
        for q in range(0, T, 2):
            a, b = hid[q, group].astype(F32), hid[q + 1, group].astype(F32)
            down = dn_out[:, q * half : (q + 2) * half]
            out_a = out_a + dot_nt(left_halves(a, b, half).astype(BF), down)
            out_b = out_b + dot_nt(right_halves(a, b, half).astype(BF), down)
        even, odd = out_a.astype(BF), out_b.astype(BF)
        keep[group] = jnp.where(p == 0, even, odd)
        away[group] = jnp.where(p == 0, odd, even)
        near_copy(group).start()

    loop(0, G, expert_out)

    def add_halves(d):
        group = (g + d) % G
        arrived(near.at[group], s_near.at[group], r_near.at[group])
        ret_send[group] = (keep[group].astype(F32) + near[group].astype(F32)).astype(BF)
        remote(
            ret_send.at[group], ret.at[g], s_ret.at[group], r_ret.at[g], 2 * group + p, t
        ).start()

    loop(1, G, add_halves)
    arrived(near.at[g], s_near.at[g], r_near.at[g])
    ret[g] = (keep[g].astype(F32) + near[g].astype(F32)).astype(BF)

    for q in range(T):
        span = slice(q * quarter, (q + 1) * quarter)
        turned_gu = rows_of(q).astype(F32).T.astype(BF)
        gate_out[:, span] = turned_gu[:half]
        up_out[:, span] = turned_gu[half:]
        sd_out[:, span] = (
            sh[q * K : (q + 1) * K, 2].reshape(quarter, C).astype(F32).T.astype(BF)
        )
    sg_out[...] = sh[:, 0].reshape(F * R, C)
    su_out[...] = sh[:, 1].reshape(F * R, C)

    def wait_part(d):
        src = (t + d) % T
        arrived(shr.at[src], s_shr.at[d], r_shr.at[src])

    loop(1, T, wait_part)
    total = shr[0].astype(F32)
    for q in range(1, T):
        total = total + shr[q].astype(F32)

    def wait_ret(d):
        src = (g + d) % G
        arrived(ret.at[src], s_ret.at[src], r_ret.at[src])

    loop(1, G, wait_ret)
    outs = ret[...].reshape(E * slots, quarter)
    for k, pick in enumerate((pick0, pick1)):
        chosen = jnp.where(pick, 1.0, 0.0).astype(BF)
        total = total + turned[:, 2 + k : 3 + k] * dot(chosen, outs)
    mixed[...] = total.astype(BF)

    def done_tp(d):
        sent(tok, s_tok.at[d], r_tok.at[0])
        sent(part.at[0], s_shr.at[d], r_shr.at[0])

        def inner(group):
            sent(hid.at[t, group], s_hid.at[d, group], r_hid.at[0, 0])

        loop(0, G, inner)

    loop(1, T, done_tp)

    def done_fs(d):
        sent(gu_send.at[0], s_gu.at[d], r_gu.at[0])

    loop(1, F, done_fs)

    def done_down(d):
        @pl.when(jnp.logical_not((d == 0) & mine))
        def _():
            sent(dn_send.at[0], s_dn.at[d], r_dn.at[0, 0])

    loop(0, F, done_down)

    def done_groups(d):
        sent(sh.at[f], s_shb.at[d], r_sh.at[0])
        sent(disp.at[0], s_db.at[d], r_port.at[0, 0])
        sent(away.at[0], s_near.at[d], r_near.at[0])

        @pl.when(d > 0)
        def _():
            sent(disp.at[0], s_da.at[d], r_port.at[0, 0])
            sent(ret_send.at[0], s_ret.at[(g + d) % G], r_ret.at[0])

        @pl.when((d >= g) & (g > 0))
        def _():
            sent(sh.at[f], s_left.at[d], r_sh.at[0])

        @pl.when((d <= g) & (g < G - 1))
        def _():
            sent(sh.at[f], s_right.at[d], r_sh.at[0])

    loop(0, G, done_groups)

    def done_blocks(block):
        for o in range(T // 2):
            sent(disp.at[0], s_in.at[o, block], r_port.at[0, 0])
            if o > 0:
                sent(disp.at[0], s_out.at[o, block], r_port.at[0, 0])

    loop(0, F, done_blocks)


def hand_on(count, *refs):
    for i in range(count):
        refs[count + i][...] = refs[i][...]


def on_device(
    tokens,
    routes,
    route_weight,
    norm_gain,
    expert_gate,
    expert_up,
    expert_down,
    shared_gate,
    shared_up,
    shared_down,
):
    F = lax.axis_size("fs")
    T = lax.axis_size("tp")
    E, R, C = expert_gate.shape
    tok_count, quarter = tokens.shape
    pick_count = routes.shape[1]
    capacity = 2 * ((3 * tok_count * pick_count + 4 * E - 1) // (4 * E))
    slots = (capacity + 15) // 16 * 16
    G, K = F // 2, F // T
    vmem = pl.BlockSpec(memory_space=pltpu.VMEM)
    dma = pltpu.SemaphoreType.DMA
    shapes = [
        (tok_count, quarter),
        (C // 2, F * R),
        (C // 2, F * R),
        (K * R, T * C // 2),
        (F * R, C),
        (F * R, C),
        (C, F * R),
    ]
    scratch = [
        (T, tok_count, quarter),
        (T, tok_count, quarter),
        (F, R, C),
        (F, R, C),
        (F, R // 2, C),
        (K, T, R // 2, C),
        (F, 3, R, C),
        (E, slots, quarter),
        (T, F, slots, quarter),
        (T, G, slots, C),
        (G, slots, quarter),
        (G, slots, quarter),
        (G, slots, quarter),
        (G, slots, quarter),
        (E, slots, quarter),
        (T, tok_count, quarter),
        (T, tok_count, quarter),
    ]
    sems = [
        (T,), (T,), (F,), (F,), (F,), (K, T), (G,), (G,), (G,), (F,), (G,), (G,),
        (T // 2, F), (T // 2, F), (T, F), (T, G), (T, G), (G,), (G,), (G,), (E,), (T,), (T,),
    ]
    results = pl.pallas_call(
        functools.partial(kernel, F, T, slots),
        out_shape=[jax.ShapeDtypeStruct(s, BF) for s in shapes],
        in_specs=[vmem] * 10,
        out_specs=[vmem] * 7,
        scratch_shapes=[pltpu.VMEM(s, BF) for s in scratch] + [dma(s) for s in sems],
        compiler_params=pltpu.CompilerParams(
            has_side_effects=True, vmem_limit_bytes=60 * 1024 * 1024
        ),
    )(
        tokens,
        routes.T,
        route_weight.T,
        norm_gain[None, :],
        expert_gate,
        expert_up,
        expert_down,
        shared_gate,
        shared_up,
        shared_down,
    )
    mixed, gate, up, down, sg, su, sd = pl.pallas_call(
        functools.partial(hand_on, 7),
        out_shape=[jax.ShapeDtypeStruct(s, BF) for s in shapes],
        in_specs=[vmem] * 7,
        out_specs=[vmem] * 7,
    )(*results)
    return (mixed, gate.T[None], up.T[None], down[None], sg, su, sd)


def solution(mesh):
    in_specs = (
        P("fs", "tp"),
        P("fs", None),
        P("fs", None),
        P("fs"),
        P(None, "fs", "tp"),
        P(None, "fs", "tp"),
        P(None, "fs", "tp"),
        P("fs", "tp"),
        P("fs", "tp"),
        P("tp", "fs"),
    )
    out_specs = (
        P("fs", "tp"),
        P("fs", None, "tp"),
        P("fs", None, "tp"),
        P("fs", "tp", None),
        P(None, "tp"),
        P(None, "tp"),
        P("tp", None),
    )
    return jax.shard_map(
        on_device, mesh=mesh, in_specs=in_specs, out_specs=out_specs, check_vma=False
    )
```

```python
import functools

import jax
import jax.numpy as jnp
from jax import lax
from jax.experimental import pallas as pl
from jax.experimental.pallas import tpu as pltpu
from jax.sharding import PartitionSpec as P

EPS = 1e-06
BF = jnp.bfloat16
F32 = jnp.float32


def loop(low, high, body):
    def step(i, carry):
        body(i)
        return carry

    lax.fori_loop(low, high, step, 0)


def dot(a, b):
    return jnp.dot(a, b, preferred_element_type=F32)


def dot_nt(a, b):
    return lax.dot_general(a, b, (((1,), (1,)), ((), ())), preferred_element_type=F32)


def left_halves(a, b, half):
    lane = lax.broadcasted_iota(jnp.int32, a.shape, 1)
    return jnp.where(lane < half, a, pltpu.roll(b, half, 1))


def right_halves(a, b, half):
    lane = lax.broadcasted_iota(jnp.int32, a.shape, 1)
    return jnp.where(lane < half, pltpu.roll(a, half, 1), b)


def silu(v):
    return v / (1.0 + jnp.exp(-v))


def kernel(
    F,
    T,
    slots,
    tok,
    routes,
    weight,
    gain,
    eg,
    eu,
    ed,
    sg,
    su,
    sd,
    mixed,
    gate_out,
    up_out,
    dn_out,
    sg_out,
    su_out,
    sd_out,
    tk,
    nm,
    gu_send,
    gu,
    dn_send,
    dn,
    sh,
    disp,
    port,
    hid,
    away,
    keep,
    near,
    ret_send,
    ret,
    part,
    shr,
    s_tok,
    r_tok,
    s_gu,
    r_gu,
    s_dn,
    r_dn,
    s_left,
    s_right,
    s_shb,
    r_sh,
    s_da,
    s_db,
    s_out,
    s_in,
    r_port,
    s_hid,
    r_hid,
    s_near,
    r_near,
    s_ret,
    r_ret,
    s_shr,
    r_shr,
):
    G = F // 2
    K = F // T
    E = eg.shape[0]
    R, C = eg.shape[1], eg.shape[2]
    half = C // 2
    tok_count = tok.shape[0]
    quarter = tok.shape[1]
    width = quarter * T
    f = lax.axis_index("fs")
    t = lax.axis_index("tp")
    g, p = f // 2, f % 2
    pair = g * 2 + (1 - p)
    t_pair = (t // 2) * 2 + (1 - t % 2)

    def remote(src, dst, send, recv, fs, tp):
        return pltpu.make_async_remote_copy(
            src_ref=src,
            dst_ref=dst,
            send_sem=send,
            recv_sem=recv,
            device_id={"fs": fs, "tp": tp},
            device_id_type=pl.DeviceIdType.MESH,
        )

    def arrived(dst, send, recv):
        remote(dst, dst, send, recv, pair, t).wait_recv()

    def sent(src, send, recv):
        remote(src, src, send, recv, pair, t).wait_send()

    def tok_copy(src, sem, to):
        return remote(tk.at[src], tk.at[src], sem, r_tok.at[src], f, to)

    for o in range(1, T // 2):
        remote(tok, tk.at[t], s_tok.at[o], r_tok.at[t], f, (t + 2 * o) % T).start()
    remote(tok, tk.at[t], s_tok.at[T // 2], r_tok.at[t], f, t_pair).start()
    tk[t] = tok[...]

    experts = lax.broadcasted_iota(jnp.int32, (tok_count, E), 1)
    line = lax.broadcasted_iota(jnp.int32, (8, tok_count), 0)
    named_by = routes[...].astype(F32)
    turned = jnp.where(line == 0, named_by[0:1], named_by[1:2])
    turned = jnp.where(line == 2, weight[0:1, :], turned)
    turned = jnp.where(line == 3, weight[1:2, :], turned).T
    first, second = turned[:, 0:1].astype(jnp.int32), turned[:, 1:2].astype(jnp.int32)
    named = ((experts == first) | (experts == second)).astype(F32)
    rows = lax.broadcasted_iota(jnp.int32, (tok_count, tok_count), 0)
    cols = lax.broadcasted_iota(jnp.int32, (tok_count, tok_count), 1)
    before = (cols < rows).astype(F32).astype(BF)
    place = dot(before, named.astype(BF))
    slot_ids = lax.broadcasted_iota(jnp.int32, (tok_count, E * slots), 1)

    def pick_of(chosen):
        spot = jnp.sum(jnp.where(experts == chosen, place, 0.0), axis=1, keepdims=True)
        return slot_ids == chosen * slots + spot.astype(jnp.int32)

    pick0, pick1 = pick_of(first), pick_of(second)
    both = jnp.where(pick0 | pick1, 1.0, 0.0).astype(BF)

    packed = lax.dot_general(
        both, tok[...], (((0,), (0,)), ((), ())), preferred_element_type=F32
    ).astype(BF)
    disp[...] = packed.reshape(E, slots, quarter)
    port[t, f] = disp[g]

    def send_disp(d):
        e = (g + d) % G
        remote(
            disp.at[e], port.at[t, f], s_da.at[d], r_port.at[t, f], 2 * e + p, t
        ).start()

    loop(1, G, send_disp)

    def shared_copy(block, sems, to):
        return remote(sh.at[block], sh.at[block], sems, r_sh.at[block], to, t)

    def share_left(block):
        @pl.when(g > 0)
        def _():
            shared_copy(block, s_left.at[block // 2], f - 2).start()

    def share_right(block):
        @pl.when(g < G - 1)
        def _():
            shared_copy(block, s_right.at[block // 2], f + 2).start()

    def share_pair(block):
        shared_copy(block, s_shb.at[block // 2], pair).start()

    def relay(k):
        @pl.when(g - k >= 0)
        def _():
            block = f - 2 * k
            arrived(sh.at[block], s_right.at[0], r_sh.at[block])
            share_right(block)
            share_pair(block)

        @pl.when(g + k < G)
        def _():
            block = f + 2 * k
            arrived(sh.at[block], s_left.at[0], r_sh.at[block])
            share_left(block)
            share_pair(block)

    def pass_block(block):
        for d in range(1, T // 2):
            remote(
                port.at[t, block],
                port.at[t, block],
                s_out.at[d, block],
                r_port.at[t, block],
                f,
                (t + 2 * d) % T,
            ).start()
        remote(
            port.at[t, block],
            port.at[t, block],
            s_in.at[0, block],
            r_port.at[t, block],
            f,
            t_pair,
        ).start()

    def direct_block(d):
        block = ((g + G - d) % G) * 2 + p

        @pl.when(d > 0)
        def _():
            arrived(port.at[t, block], s_da.at[d], r_port.at[t, block])

        remote(
            port.at[t, block],
            port.at[t, block],
            s_db.at[d],
            r_port.at[t, block],
            pair,
            t,
        ).start()
        pass_block(block)

    def pair_block(d):
        block = ((g + G - d) % G) * 2 + 1 - p
        arrived(port.at[t, block], s_db.at[d], r_port.at[t, block])
        pass_block(block)

    def inner_block(d):
        for o in range(1, T // 2):
            src = (t + 2 * o) % T
            for q in (p, 1 - p):
                block = ((g + G - d) % G) * 2 + q
                arrived(port.at[src, block], s_out.at[o, block], r_port.at[src, block])
                remote(
                    port.at[src, block],
                    port.at[src, block],
                    s_in.at[o, block],
                    r_port.at[src, block],
                    f,
                    t_pair,
                ).start()

    loop(0, 1, direct_block)

    gains = jnp.broadcast_to(gain[...], (8, R)).T[:, 0:1]

    def fold(e):
        gate, up = eg[e] * gains, eu[e] * gains
        gu_send[2 * e] = left_halves(gate, up, half).astype(BF)
        gu_send[2 * e + 1] = right_halves(gate, up, half).astype(BF)

    loop(0, E, fold)
    gu[f] = gu_send[f]

    def send_gu(d):
        j = (f + d) % F
        remote(gu_send.at[j], gu.at[f], s_gu.at[d], r_gu.at[f], j, t).start()

    loop(1, F, send_gu)

    def fold_down(e):
        top, low = ed[e, : R // 2], ed[e, R // 2 :]
        dn_send[2 * e] = left_halves(top, low, half).astype(BF)
        dn_send[2 * e + 1] = right_halves(top, low, half).astype(BF)

    loop(0, E, fold_down)
    sh[f, 0] = (sg[...] * gains).astype(BF)
    sh[f, 1] = (su[...] * gains).astype(BF)
    sh[f, 2] = sd[...].T.astype(BF)

    def down_copy(d):
        j = (f + d) % F
        return remote(
            dn_send.at[j], dn.at[f % K, t], s_dn.at[d], r_dn.at[f % K, t], j, f // K
        )

    mine = f // K == t

    @pl.when(mine)
    def _():
        dn[f % K, t] = dn_send[f]

    def send_down(d):
        @pl.when(jnp.logical_not((d == 0) & mine))
        def _():
            down_copy(d).start()

    loop(0, F, send_down)
    share_left(f)
    share_right(f)
    loop(1, G, direct_block)
    loop(0, G, pair_block)
    share_pair(f)
    loop(0, G, inner_block)

    for o in range(1, T // 2):
        src = (t + 2 * o) % T
        arrived(tk.at[src], s_tok.at[o], r_tok.at[src])
        tok_copy(src, s_tok.at[T // 2 + o], t_pair).start()

    def wait_gu(d):
        src = (f + d) % F
        arrived(gu.at[src], s_gu.at[d], r_gu.at[src])

    loop(1, F, wait_gu)

    def rows_of(q):
        return gu[q * K : (q + 1) * K].reshape(quarter, C)

    def hidden_of(block):
        total = jnp.zeros((slots, C), F32)
        squares = jnp.zeros((slots, 1), F32)
        for q in range(T):
            total = total + dot(port[q, block], rows_of(q))
            x = port[q, block].astype(F32)
            squares = squares + jnp.sum(x * x, axis=1, keepdims=True)
        total = total * lax.rsqrt(squares / width + EPS)
        return silu(total) * pltpu.roll(total, half, 1)

    def wait_inner(block):
        for o in range(T // 2):
            src = (t_pair + 2 * o) % T
            arrived(port.at[src, block], s_in.at[o, block], r_port.at[src, block])

    def expert_hidden(d):
        group = (g + G - d) % G
        wait_inner(2 * group)
        wait_inner(2 * group + 1)
        hid[t, group] = left_halves(
            hidden_of(2 * group), hidden_of(2 * group + 1), half
        ).astype(BF)
        for o in range(1, T):
            remote(
                hid.at[t, group],
                hid.at[t, group],
                s_hid.at[o, group],
                r_hid.at[t, group],
                f,
                (t + o) % T,
            ).start()

    loop(0, G, expert_hidden)

    loop(1, min(2, G), relay)

    def wait_down(k):
        for q in range(T):

            @pl.when(jnp.logical_not((t * K + k == f) & (t == q)))
            def _():
                arrived(dn.at[k, q], s_dn.at[0], r_dn.at[k, q])

    loop(0, K, wait_down)

    def place_down(k):
        for q in range(0, T, 2):
            a, b = dn[k, q].astype(F32), dn[k, q + 1].astype(F32)
            block = jnp.concatenate([left_halves(a, b, half), right_halves(a, b, half)], axis=0)
            dn_out[pl.ds(pl.multiple_of(k * R, R), R), q * half : (q + 2) * half] = block.astype(BF)

    loop(0, K, place_down)

    def near_copy(group):
        return remote(
            away.at[group], near.at[group], s_near.at[group], r_near.at[group], pair, t
        )

    def expert_out(d):
        group = (g + G - d) % G
        for o in range(1, T):
            src = (t + o) % T
            arrived(hid.at[src, group], s_hid.at[o, group], r_hid.at[src, group])
        out_a = jnp.zeros((slots, quarter), F32)
        out_b = jnp.zeros((slots, quarter), F32)
        for q in range(0, T, 2):
            a, b = hid[q, group].astype(F32), hid[q + 1, group].astype(F32)
            down = dn_out[:, q * half : (q + 2) * half]
            out_a = out_a + dot_nt(left_halves(a, b, half).astype(BF), down)
            out_b = out_b + dot_nt(right_halves(a, b, half).astype(BF), down)
        even, odd = out_a.astype(BF), out_b.astype(BF)
        keep[group] = jnp.where(p == 0, even, odd)
        away[group] = jnp.where(p == 0, odd, even)
        near_copy(group).start()

    loop(0, G, expert_out)
    loop(2, min(3, G), relay)

    def add_halves(d):
        group = (g + d) % G
        arrived(near.at[group], s_near.at[group], r_near.at[group])
        ret_send[group] = (keep[group].astype(F32) + near[group].astype(F32)).astype(BF)
        remote(
            ret_send.at[group], ret.at[g], s_ret.at[group], r_ret.at[g], 2 * group + p, t
        ).start()

    loop(1, G, add_halves)
    arrived(near.at[g], s_near.at[g], r_near.at[g])
    ret[g] = (keep[g].astype(F32) + near[g].astype(F32)).astype(BF)

    def wait_shared(d):
        block = ((g + G - d) % G) * 2 + 1 - p
        arrived(sh.at[block], s_shb.at[d], r_sh.at[block])

    loop(3, G, relay)
    loop(0, G, wait_shared)

    for o in range(T // 2):
        src = (t_pair + 2 * o) % T
        arrived(tk.at[src], s_tok.at[o], r_tok.at[src])
    squares = jnp.zeros((tok_count, 1), F32)
    for q in range(T):
        x = tk[q].astype(F32)
        squares = squares + jnp.sum(x * x, axis=1, keepdims=True)
    scale = lax.rsqrt(squares / width + EPS)
    for q in range(T):
        nm[q] = (tk[q].astype(F32) * scale).astype(BF)

    gate_sh = sh[:, 0].reshape(F * R, C)
    up_sh = sh[:, 1].reshape(F * R, C)
    down_sh = sh[:, 2].reshape(F * R, C)
    act = jnp.zeros((tok_count, C), F32)
    lin = jnp.zeros((tok_count, C), F32)
    for q in range(T):
        act = act + dot(nm[q], gate_sh[q * quarter : (q + 1) * quarter])
        lin = lin + dot(nm[q], up_sh[q * quarter : (q + 1) * quarter])
    hidden_sh = (silu(act) * lin).astype(BF)
    for q in range(T):
        part[q] = dot_nt(hidden_sh, down_sh[q * quarter : (q + 1) * quarter]).astype(BF)
    shr[t] = part[t]

    def send_part(d):
        q = (t + d) % T
        remote(part.at[q], shr.at[t], s_shr.at[d], r_shr.at[t], f, q).start()

    loop(1, T, send_part)

    for q in range(T):
        span = slice(q * quarter, (q + 1) * quarter)
        turned_gu = rows_of(q).astype(F32).T.astype(BF)
        gate_out[:, span] = turned_gu[:half]
        up_out[:, span] = turned_gu[half:]
        sd_out[:, span] = (
            sh[q * K : (q + 1) * K, 2].reshape(quarter, C).astype(F32).T.astype(BF)
        )
    sg_out[...] = sh[:, 0].reshape(F * R, C)
    su_out[...] = sh[:, 1].reshape(F * R, C)

    def wait_part(d):
        src = (t + d) % T
        arrived(shr.at[src], s_shr.at[d], r_shr.at[src])

    loop(1, T, wait_part)
    total = shr[0].astype(F32)
    for q in range(1, T):
        total = total + shr[q].astype(F32)

    def wait_ret(d):
        src = (g + d) % G
        arrived(ret.at[src], s_ret.at[src], r_ret.at[src])

    loop(1, G, wait_ret)
    outs = ret[...].reshape(E * slots, quarter)
    for k, pick in enumerate((pick0, pick1)):
        chosen = jnp.where(pick, 1.0, 0.0).astype(BF)
        total = total + turned[:, 2 + k : 3 + k] * dot(chosen, outs)
    mixed[...] = total.astype(BF)

    def done_tp(d):
        sent(tok, s_tok.at[d], r_tok.at[0])
        sent(part.at[0], s_shr.at[d], r_shr.at[0])

        def inner(group):
            sent(hid.at[t, group], s_hid.at[d, group], r_hid.at[0, 0])

        loop(0, G, inner)

    loop(1, T, done_tp)

    def done_fs(d):
        sent(gu_send.at[0], s_gu.at[d], r_gu.at[0])

    loop(1, F, done_fs)

    def done_down(d):
        @pl.when(jnp.logical_not((d == 0) & mine))
        def _():
            sent(dn_send.at[0], s_dn.at[d], r_dn.at[0, 0])

    loop(0, F, done_down)

    def done_groups(d):
        sent(sh.at[f], s_shb.at[d], r_sh.at[0])
        sent(disp.at[0], s_db.at[d], r_port.at[0, 0])
        sent(away.at[0], s_near.at[d], r_near.at[0])

        @pl.when(d > 0)
        def _():
            sent(disp.at[0], s_da.at[d], r_port.at[0, 0])
            sent(ret_send.at[0], s_ret.at[(g + d) % G], r_ret.at[0])

        @pl.when((d >= g) & (g > 0))
        def _():
            sent(sh.at[f], s_left.at[d], r_sh.at[0])

        @pl.when((d <= g) & (g < G - 1))
        def _():
            sent(sh.at[f], s_right.at[d], r_sh.at[0])

    loop(0, G, done_groups)

    def done_blocks(block):
        for o in range(T // 2):
            sent(disp.at[0], s_in.at[o, block], r_port.at[0, 0])
            if o > 0:
                sent(disp.at[0], s_out.at[o, block], r_port.at[0, 0])

    loop(0, F, done_blocks)


def hand_on(count, *refs):
    for i in range(count):
        refs[count + i][...] = refs[i][...]


def on_device(
    tokens,
    routes,
    route_weight,
    norm_gain,
    expert_gate,
    expert_up,
    expert_down,
    shared_gate,
    shared_up,
    shared_down,
):
    F = lax.axis_size("fs")
    T = lax.axis_size("tp")
    E, R, C = expert_gate.shape
    tok_count, quarter = tokens.shape
    pick_count = routes.shape[1]
    capacity = 2 * ((3 * tok_count * pick_count + 4 * E - 1) // (4 * E))
    slots = (capacity + 15) // 16 * 16
    G, K = F // 2, F // T
    vmem = pl.BlockSpec(memory_space=pltpu.VMEM)
    dma = pltpu.SemaphoreType.DMA
    shapes = [
        (tok_count, quarter),
        (C // 2, F * R),
        (C // 2, F * R),
        (K * R, T * C // 2),
        (F * R, C),
        (F * R, C),
        (C, F * R),
    ]
    scratch = [
        (T, tok_count, quarter),
        (T, tok_count, quarter),
        (F, R, C),
        (F, R, C),
        (F, R // 2, C),
        (K, T, R // 2, C),
        (F, 3, R, C),
        (E, slots, quarter),
        (T, F, slots, quarter),
        (T, G, slots, C),
        (G, slots, quarter),
        (G, slots, quarter),
        (G, slots, quarter),
        (G, slots, quarter),
        (E, slots, quarter),
        (T, tok_count, quarter),
        (T, tok_count, quarter),
    ]
    sems = [
        (T,), (T,), (F,), (F,), (F,), (K, T), (G,), (G,), (G,), (F,), (G,), (G,),
        (T // 2, F), (T // 2, F), (T, F), (T, G), (T, G), (G,), (G,), (G,), (E,), (T,), (T,),
    ]
    results = pl.pallas_call(
        functools.partial(kernel, F, T, slots),
        out_shape=[jax.ShapeDtypeStruct(s, BF) for s in shapes],
        in_specs=[vmem] * 10,
        out_specs=[vmem] * 7,
        scratch_shapes=[pltpu.VMEM(s, BF) for s in scratch] + [dma(s) for s in sems],
        compiler_params=pltpu.CompilerParams(
            has_side_effects=True, vmem_limit_bytes=60 * 1024 * 1024
        ),
    )(
        tokens,
        routes.T,
        route_weight.T,
        norm_gain[None, :],
        expert_gate,
        expert_up,
        expert_down,
        shared_gate,
        shared_up,
        shared_down,
    )
    mixed, gate, up, down, sg, su, sd = pl.pallas_call(
        functools.partial(hand_on, 7),
        out_shape=[jax.ShapeDtypeStruct(s, BF) for s in shapes],
        in_specs=[vmem] * 7,
        out_specs=[vmem] * 7,
    )(*results)
    return (mixed, gate.T[None], up.T[None], down[None], sg, su, sd)


def solution(mesh):
    in_specs = (
        P("fs", "tp"),
        P("fs", None),
        P("fs", None),
        P("fs"),
        P(None, "fs", "tp"),
        P(None, "fs", "tp"),
        P(None, "fs", "tp"),
        P("fs", "tp"),
        P("fs", "tp"),
        P("tp", "fs"),
    )
    out_specs = (
        P("fs", "tp"),
        P("fs", None, "tp"),
        P("fs", None, "tp"),
        P("fs", "tp", None),
        P(None, "tp"),
        P(None, "tp"),
        P("tp", None),
    )
    return jax.shard_map(
        on_device, mesh=mesh, in_specs=in_specs, out_specs=out_specs, check_vma=False
    )
```
